32 devices in a mesh: ep: 16 (over z, y, x), tp: 2 (over core).
Axes of the slice: x: 2, y: 2, z: 4, core: 2. Of those that a mesh axis runs over, the one named last changes fastest.
Arguments:
- tokens: bfloat16 [256, 2048], P('ep'), may hold values from -6 to 6
- cache_keys: bfloat16 [256, 2, 64, 1024], P('ep', 'tp'), may hold values from -6 to 6
- cache_values: bfloat16 [256, 2, 64, 1024], P('ep', 'tp'), may hold values from -6 to 6
- cache_lengths: int32 [256], P('ep'), may hold values from 1 to 1024, as said below
- norm_in: float32 [2048], replicated, may hold values from 0.1 to 1.9
- w_query: bfloat16 [2048, 512], P(None, 'tp'), may hold values from -0.125 to 0.125
- w_key: bfloat16 [2048, 128], P(None, 'tp'), may hold values from -0.125 to 0.125
- w_value: bfloat16 [2048, 128], P(None, 'tp'), may hold values from -0.125 to 0.125
- stick_bias: float32 [8], P('tp'), may hold values from -8 to -1.5
- w_output: bfloat16 [512, 2048], P('tp'), may hold values from -0.75 to 0.75
- norm_mid: float32 [2048], replicated, may hold values from 0.1 to 1.9
- routes: int32 [256, 6], P('ep'), may hold values from 0 to 15, all different within a row; in each aligned block of 16 rows (0 to 15, 16 to 31, ...) at most 6 rows name the same one
- route_weights: float32 [256, 6], P('ep'), may hold values from 0.1 to 1
- expert_gate: bfloat16 [16, 2048, 512], P('ep', None, 'tp'), may hold values from -0.125 to 0.125
- expert_up: bfloat16 [16, 2048, 512], P('ep', None, 'tp'), may hold values from -0.125 to 0.125
- expert_down: bfloat16 [16, 512, 2048], P('ep', 'tp'), may hold values from -0.25 to 0.25
- dense_gate: bfloat16 [2048, 256], P('ep'), may hold values from -0.125 to 0.125
- dense_up: bfloat16 [2048, 256], P('ep'), may hold values from -0.125 to 0.125
- dense_down: bfloat16 [256, 2048], P(None, 'ep'), may hold values from -0.375 to 0.375
- mix_gate: float32 [2048], replicated, may hold values from -0.125 to 0.125
- norm_out: float32 [2048], replicated, may hold values from 0.1 to 1.9
Outputs:
- mixed: bfloat16 [256, 2048], P('ep')
- fresh_keys: bfloat16 [256, 128], P('ep', 'tp')
- fresh_values: bfloat16 [256, 128], P('ep', 'tp')
The draws below stay inside these ranges and needn't reach their ends.
Inputs may be any that keep to these rules, and one draw needn't show every extreme that they name: `cache_lengths`: positions at or past a sequence's length are not read. Among the sequences of one index of ep some sequence has length 1024. `routes`: each row names 6 different experts; among the rows of one index of ep (aligned blocks of 16 rows) no expert is named by more than 6 rows, and that bound is reached.
All inputs are finite; a program needn't handle non-finite values.
Results may differ from the reference program's by a relative error of at most 0.015.
Values may be sent and summed in bfloat16 or wider, within the bound.
A program may use at most 64 MiB of HBM per device.

```python
import math
import jax
import jax.numpy as jnp
import numpy as np
from jax import lax

D = 2048
HEADS = 8
KVH = 2
HD = 64
EW = 512
SHARED = 256
TOPK = 6
SEQ_DEV = 16
CACHE = 1024
SEQS = 256
EXPERTS = 16
CAP = 6
N_EP = 16
N_TP = 2


def draw_cache_lengths(key, part):
    first_key, second_key = jax.random.split(jax.random.fold_in(key, 11))
    drawn_lengths = jax.random.randint(first_key, (SEQS,), 1, CACHE + 1)
    chosen = jax.random.randint(second_key, (SEQS // SEQ_DEV,), 0, SEQ_DEV)
    position = jnp.arange(SEQS)
    is_full = position % SEQ_DEV == jnp.repeat(chosen, SEQ_DEV)
    return jnp.where(is_full, CACHE, drawn_lengths).astype(jnp.int32)


def draw_stick_bias(key, part):
    first_key, second_key, third_key = jax.random.split(jax.random.fold_in(key, 23), 3)
    is_fast = jax.random.randint(first_key, (HEADS,), 0, 2) == 1
    fast_bias = jax.random.uniform(second_key, (HEADS,), jnp.float32, -2.5, -1.5)
    slow_bias = jax.random.uniform(third_key, (HEADS,), jnp.float32, -7.5, -6.0)
    return jnp.where(is_fast, fast_bias, slow_bias).astype(jnp.float32)


def shard_levels(rng, shape, cuts, least, largest):
    loudness, own = 1.0, jax.random.fold_in(rng, 6)
    for dim, shards_of in cuts:
        draws = jnp.exp(jax.random.uniform(jax.random.fold_in(own, dim), (shards_of,), jnp.float32, least / len(cuts), largest / len(cuts)))
        loudness = loudness * jnp.repeat(draws, shape[dim] // shards_of).reshape([-1 if axis == dim else 1 for axis in range(len(shape))])
    return loudness


def deal_out(rng, own, number, rows, amount, top, most, slope):
    sequence = jax.random.permutation(rng, amount)
    packed, ordinary = portions_of(amount, rows * top, most, slope, True), portions_of(amount, rows * top, most, slope, False)
    places = jnp.arange(amount)

    def named(sizes, offset_by):
        used = int((sizes > 0).sum())
        fixed = max(1, used // 4)
        shifted = fixed + (places - fixed + offset_by * (used - fixed)) % max(1, amount - fixed)
        return jnp.zeros((amount,), jnp.int32).at[sequence[jnp.where(places < fixed, places, shifted)]].set(jnp.asarray(sizes, jnp.int32))

    sizes = jnp.where(number % 4 == 0, named(packed, number // 4), named(ordinary, number - number // 4 - 1))
    mixed = jax.random.permutation(jax.random.fold_in(own, 3), amount)
    donor, receiver = mixed[0:amount // 2 * 2:2], mixed[1:amount // 2 * 2:2]
    slack = jnp.minimum(sizes[donor] - 1, most - sizes[receiver]) // 2
    slack = jnp.where((donor == sequence[0]) | (receiver == sequence[0]) | (sizes[receiver] == 0), 0, jnp.maximum(slack, 0))
    shifted = jax.random.randint(jax.random.fold_in(own, 4), (amount // 2,), 0, 1 << 20) % (slack + 1)
    sizes = sizes.at[donor].add(-shifted).at[receiver].add(shifted)
    members = jnp.searchsorted(jnp.cumsum(sizes), jnp.arange(rows * top), side="right").astype(jnp.int32)
    table = members.reshape(top, rows).T
    table = table[jax.random.permutation(jax.random.fold_in(own, 1), rows)]
    offset_by = jax.random.randint(jax.random.fold_in(own, 2), (rows, 1), 0, top)
    return jnp.take_along_axis(table, (jnp.arange(top)[None, :] + offset_by) % top, axis=1)


def portions_of(amount, total, most, slope, full):
    loads = [(1 << 20) // math.isqrt(rank ** slope) + 1 for rank in range(1, amount + 1)]
    largest = most if full else min(most, max(-(-total // amount), total * loads[0] // sum(loads)))
    least = 1 if total - largest >= amount - 1 else 0
    given, surplus = [largest] + [least] * (amount - 1), total - largest - least * (amount - 1)
    while surplus > 0:
        free = [i for i in range(1, amount) if given[i] < largest] or [i for i in range(1, amount) if given[i] < most]
        pool, remaining = sum([loads[i] for i in free]), surplus
        for i in free:
            extra = min(most - given[i], max(1, remaining * loads[i] // pool), surplus)
            given[i] = given[i] + extra
            surplus = surplus - extra
    return np.array(given)


def noise(rng, shape, deviation, reach, pieces=(), kind=jnp.bfloat16):
    level = shard_levels(rng, shape, pieces, -0.22, 0.18) if pieces else 1.0
    entries = jax.random.normal(rng, shape, jnp.float32) * deviation * level
    return jnp.minimum(jnp.maximum(entries, -reach), reach).astype(kind)


def setup_inputs(seed: int = 0) -> dict:
    arg_keys = jax.random.split(jax.random.key(seed), 22)
    tokens = noise(arg_keys[0], (SEQS, D), 1.0, 6.0, ((0, 16),))
    cache_keys = noise(arg_keys[1], (SEQS, KVH, HD, CACHE), 1.0, 6.0, ((0, 16), (1, 2)))
    cache_values = noise(arg_keys[2], (SEQS, KVH, HD, CACHE), 1.0, 6.0, ((0, 16), (1, 2)))
    cache_lengths = draw_cache_lengths(jax.random.fold_in(arg_keys[21], 71), 0)
    norm_in = jnp.clip(1.0 + 0.18 * jax.random.normal(arg_keys[4], (D,), jnp.float32), 0.1, 1.9)
    w_query = noise(arg_keys[5], (D, HEADS * HD), D ** -0.5, 0.125, ((1, 2),))
    w_key = noise(arg_keys[6], (D, KVH * HD), D ** -0.5, 0.125, ((1, 2),))
    w_value = noise(arg_keys[7], (D, KVH * HD), D ** -0.5, 0.125, ((1, 2),))
    stick_bias = draw_stick_bias(jax.random.fold_in(arg_keys[21], 71), 0)
    w_output = noise(arg_keys[9], (HEADS * HD, D), HD ** -0.5, 0.75, ((0, 2),))
    norm_mid = jnp.clip(1.0 + 0.18 * jax.random.normal(arg_keys[10], (D,), jnp.float32), 0.1, 1.9)
    routes_keys = jax.random.split(jax.random.fold_in(arg_keys[11], 1), SEQS // SEQ_DEV)
    routes_turns = jax.random.permutation(jax.random.fold_in(arg_keys[11], 3), SEQS // SEQ_DEV)
    routes = jax.vmap(lambda own, number: deal_out(jax.random.fold_in(arg_keys[11], 2), own, number, SEQ_DEV, EXPERTS, TOPK, CAP, 1))(routes_keys, routes_turns).reshape((SEQS, TOPK))
    route_weights = jnp.clip(jnp.exp(math.log(1.0) - 2.3025851 * jax.random.uniform(arg_keys[12], (SEQS, TOPK), jnp.float32) ** shard_levels(arg_keys[12], (SEQS, TOPK), ((0, 16),), -0.2, 0.2)), 0.1, 1.0)
    expert_gate = noise(arg_keys[13], (EXPERTS, D, EW), D ** -0.5, 0.125, ((0, 16), (2, 2)))
    expert_up = noise(arg_keys[14], (EXPERTS, D, EW), D ** -0.5, 0.125, ((0, 16), (2, 2)))
    expert_down = noise(arg_keys[15], (EXPERTS, EW, D), EW ** -0.5, 0.25, ((0, 16), (1, 2)))
    dense_gate = noise(arg_keys[16], (D, SHARED), D ** -0.5, 0.125, ((0, 16),))
    dense_up = noise(arg_keys[17], (D, SHARED), D ** -0.5, 0.125, ((0, 16),))
    dense_down = noise(arg_keys[18], (SHARED, D), SHARED ** -0.5, 0.375, ((1, 16),))
    mix_gate = noise(arg_keys[19], (D,), D ** -0.5, 0.125, (), jnp.float32)
    norm_out = jnp.clip(1.0 + 0.18 * jax.random.normal(arg_keys[20], (D,), jnp.float32), 0.1, 1.9)
    return dict(tokens=tokens, cache_keys=cache_keys, cache_values=cache_values, cache_lengths=cache_lengths, norm_in=norm_in, w_query=w_query, w_key=w_key, w_value=w_value, stick_bias=stick_bias, w_output=w_output, norm_mid=norm_mid, routes=routes, route_weights=route_weights, expert_gate=expert_gate, expert_up=expert_up, expert_down=expert_down, dense_gate=dense_gate, dense_up=dense_up, dense_down=dense_down, mix_gate=mix_gate, norm_out=norm_out)


def layer_norm(values, gain):
    floats = values.astype(jnp.float32)
    center = lax.optimization_barrier(jnp.mean(floats, -1, keepdims=True))
    spread = lax.optimization_barrier(jnp.mean(jnp.square(floats - center), -1, keepdims=True))
    return (floats - center) * lax.rsqrt(spread + 1e-05) * gain

def rounded(values):
    return lax.optimization_barrier(values.astype(jnp.bfloat16)).astype(jnp.float32)

def reference(tokens, cache_keys, cache_values, cache_lengths, norm_in, w_query, w_key, w_value, stick_bias, w_output, norm_mid, routes, route_weights, expert_gate, expert_up, expert_down, dense_gate, dense_up, dense_down, mix_gate, norm_out):
    normed = layer_norm(tokens, norm_in).astype(jnp.bfloat16)
    queries = jnp.dot(normed, w_query, preferred_element_type=jnp.float32).astype(jnp.bfloat16)
    fresh_keys = jnp.dot(normed, w_key, preferred_element_type=jnp.float32).astype(jnp.bfloat16)
    fresh_values = jnp.dot(normed, w_value, preferred_element_type=jnp.float32).astype(jnp.bfloat16)
    groups = HEADS // KVH
    bias_grid = stick_bias.astype(jnp.float32).reshape(KVH, groups)

    def attend(inputs):
        query_block, key_block, value_block, length_block = inputs
        query_grid = query_block.reshape(SEQ_DEV, KVH, groups, HD).astype(jnp.float32)
        scores = jnp.einsum('bkgd,bkdc->bkgc', query_grid, key_block.astype(jnp.float32)) * HD ** (-0.5)
        scores = scores + bias_grid[None, :, :, None]
        visible = (jnp.arange(CACHE)[None, :] < length_block[:, None])[:, None, None, :]
        log_keep = jnp.where(visible, jax.nn.log_sigmoid(-scores), 0.0)
        later_sum = lax.cumsum(log_keep, axis=3, reverse=True) - log_keep
        stick = jnp.where(visible, jnp.exp(jax.nn.log_sigmoid(scores) + later_sum), 0.0).astype(jnp.bfloat16)
        output = jnp.einsum('bkgc,bkdc->bkgd', stick.astype(jnp.float32), value_block.astype(jnp.float32))
        return output.reshape(SEQ_DEV, HEADS * HD).astype(jnp.bfloat16)
    block_count = SEQS // SEQ_DEV
    attended = lax.map(attend, (queries.reshape(block_count, SEQ_DEV, HEADS * HD), cache_keys.reshape(block_count, SEQ_DEV, KVH, HD, CACHE), cache_values.reshape(block_count, SEQ_DEV, KVH, HD, CACHE), cache_lengths.reshape(block_count, SEQ_DEV)))
    attended = attended.reshape(SEQS, HEADS * HD)
    projected = jnp.dot(attended, w_output, preferred_element_type=jnp.float32)
    hidden = layer_norm(normed.astype(jnp.float32) + projected, norm_mid).astype(jnp.bfloat16)
    slots = N_EP * CAP
    part_width = EW // N_TP

    def run_expert(inputs):
        number, gate_w, up_w, down_w = inputs
        is_hit = routes == number
        weight_sum = lax.optimization_barrier(jnp.sum(jnp.where(is_hit, route_weights, 0.0), axis=1))
        is_used = jnp.any(is_hit, axis=1)
        picked = jnp.nonzero(is_used, size=slots, fill_value=0)[0].astype(jnp.int32)
        is_valid = (jnp.arange(slots) < jnp.sum(is_used.astype(jnp.int32))).astype(weight_sum.dtype)
        token_rows = hidden[picked]
        gate_pre = jnp.dot(token_rows, gate_w, preferred_element_type=jnp.float32)
        up_pre = jnp.dot(token_rows, up_w, preferred_element_type=jnp.float32)
        act = (jax.nn.silu(gate_pre) * up_pre).astype(jnp.bfloat16)
        combined = jnp.zeros((slots, D), gate_pre.dtype)
        for index in range(N_TP):
            partial_value = jnp.dot(act[:, index * part_width:(index + 1) * part_width], down_w[index * part_width:(index + 1) * part_width], preferred_element_type=jnp.float32)
            combined = combined + rounded(partial_value)
        expert_out = rounded(combined)
        return (picked, expert_out * (weight_sum[picked] * is_valid)[:, None])
    picked_all, terms = lax.map(run_expert, (jnp.arange(EXPERTS).astype(jnp.int32), expert_gate, expert_up, expert_down))
    routed = jax.ops.segment_sum(terms.reshape(-1, D), picked_all.reshape(-1), num_segments=SEQS)
    dense_pre = jnp.dot(hidden, dense_gate, preferred_element_type=jnp.float32)
    dense_lin = jnp.dot(hidden, dense_up, preferred_element_type=jnp.float32)
    dense_act = (jax.nn.silu(dense_pre) * dense_lin).astype(jnp.bfloat16)
    dense_out = jnp.dot(dense_act, dense_down, preferred_element_type=jnp.float32)
    mix_weight = jax.nn.sigmoid(jnp.dot(hidden.astype(jnp.float32), mix_gate, precision=lax.Precision.HIGHEST))
    combined_rows = hidden.astype(jnp.float32) + routed + mix_weight[:, None] * dense_out
    mixed = layer_norm(combined_rows, norm_out).astype(jnp.bfloat16)
    return (mixed, fresh_keys, fresh_values)
```

```python
import functools

import jax
import jax.numpy as jnp
from jax import lax
from jax.experimental import pallas as pl
from jax.experimental.pallas import tpu as pltpu
from jax.sharding import PartitionSpec as P

MESH = pl.DeviceIdType.MESH
F32 = jnp.float32
BF16 = jnp.bfloat16
LANES = 128


def layer_norm(values, gain):
    center = jnp.mean(values, -1, keepdims=True)
    spread = jnp.mean(jnp.square(values - center), -1, keepdims=True)
    return (values - center) * lax.rsqrt(spread + 1e-05) * gain


def sigmoid(x):
    return 1.0 / (1.0 + jnp.exp(-x))


def iota(shape, dim):
    return lax.broadcasted_iota(jnp.int32, shape, dim)


def bits(n):
    assert n & (n - 1) == 0
    return n.bit_length() - 1


def dot(a, b):
    return jnp.dot(a, b, preferred_element_type=F32)


def dot_nt(a, b):
    return lax.dot_general(a, b, (((1,), (1,)), ((), ())), preferred_element_type=F32)


def dot_tn(a, b):
    return lax.dot_general(a, b, (((0,), (0,)), ((), ())), preferred_element_type=F32)


def layer_kernel(
    ep, slots, chunks, head_dim,
    tokens, norm_in, norm_mid, norm_out, mix_gate, routes, route_weights, lengths, bias,
    wq, wk, wv, keys, values, wo, eg, eu, ed, dg, du, dd,
    mixed, fresh_k, fresh_v,
    wq_v, wk_v, wv_v, k_v, v_v, wo_v, eg_v, eu_v, ed_v, dd_v,
    pack, gath, proj_out, proj_in, outgoing, received, expert_y, returned, fin_out, fin_in,
    load_sem, own_sem, gs, gr, ds, dr, rs, rr, ts, tr,
):
    me = lax.axis_index("ep")
    core = lax.axis_index("tp")
    other = 1 - core
    seqs, width = tokens.shape
    heads = bias.shape[0]
    length = keys.shape[1]
    rows = dg.shape[0]
    share = pack.shape[2]

    barrier = pltpu.get_barrier_semaphore()

    def greet(p, c):
        pl.semaphore_signal(
            barrier, inc=1, device_id=(lax.rem(me + p, ep), core), device_id_type=MESH
        )
        return c

    lax.fori_loop(1, ep, greet, 0)
    pl.semaphore_signal(barrier, inc=1, device_id=(me, other), device_id_type=MESH)

    offset = pl.multiple_of(core * share, share)
    span = keys.shape[0] // chunks
    moves = [
        (dd.at[pl.ds(offset, share), :], dd_v),
        (dg.at[:, pl.ds(offset, share)], pack.at[0]),
        (du.at[:, pl.ds(offset, share)], pack.at[1]),
        (wq, wq_v),
    ]
    moves += [(keys.at[pl.ds(c * span, span)], k_v.at[pl.ds(c * span, span)]) for c in range(chunks)]
    moves += [(values.at[pl.ds(c * span, span)], v_v.at[pl.ds(c * span, span)]) for c in range(chunks)]
    moves += [(wo, wo_v), (wk, wk_v), (wv, wv_v), (eg, eg_v), (eu, eu_v), (ed, ed_v)]
    loads = [pltpu.make_async_copy(a, b, load_sem.at[i]) for i, (a, b) in enumerate(moves)]
    for load in loads:
        load.start()
    key_loads = loads[4 : 4 + chunks]
    value_loads = loads[4 + chunks : 4 + 2 * chunks]
    wo_load, wk_load, wv_load, eg_load, eu_load, ed_load = loads[4 + 2 * chunks :]

    normed = layer_norm(tokens[...].astype(F32), norm_in[...]).astype(BF16)

    for load in loads[:3]:
        load.wait()
    pack[2] = dd_v[...].astype(F32).T.astype(BF16)

    def block(index, size):
        return pl.ds(pl.multiple_of(index * size, size), size)

    pl.semaphore_wait(barrier, ep)

    def gather(p, target):
        return pltpu.make_async_remote_copy(
            src_ref=pack,
            dst_ref=gath.at[:, block(target, rows), :],
            send_sem=gs.at[p],
            recv_sem=gr.at[p],
            device_id=(lax.rem(me + p, ep), core),
            device_id_type=MESH,
        )

    def start_gather(p, c):
        gather(p, me).start()
        return c

    lax.fori_loop(1, ep, start_gather, 0)
    own_gather = pltpu.make_async_copy(pack, gath.at[:, block(me, rows), :], own_sem.at[0])
    own_gather.start()

    total = ep * slots
    slot_of = iota((seqs, total), 1)
    expert_of = lax.shift_right_logical(slot_of, bits(slots))
    place_of = slot_of & (slots - 1)
    route_rows = routes[...]
    weight_rows = route_weights[...]
    member = jnp.zeros((seqs, total), F32)
    weight = jnp.zeros((seqs, total), F32)
    for k in range(route_rows.shape[1]):
        hit = route_rows[:, k : k + 1] == expert_of
        member = jnp.where(hit, 1.0, member)
        weight = jnp.where(hit, weight_rows[:, k : k + 1], weight)
    earlier = jnp.where(iota((seqs, seqs), 0) > iota((seqs, seqs), 1), 1.0, 0.0).astype(BF16)
    before = dot(earlier, member.astype(BF16)).astype(jnp.int32)
    chosen = jnp.where(before == place_of, member, 0.0)
    weight = weight * chosen
    chosen = chosen.astype(BF16)
    w_hi = weight.astype(BF16)
    w_rest = weight - w_hi.astype(F32)
    w_mid = w_rest.astype(BF16)
    w_lo = (w_rest - w_mid.astype(F32)).astype(BF16)
    weight_split = jnp.concatenate([w_hi.astype(F32), w_mid.astype(F32), w_lo.astype(F32)], axis=0).astype(BF16)

    grid_rows = heads * seqs
    flat = heads * head_dim
    col = iota((flat, heads * LANES), 1)
    spread_table = jnp.where(
        iota((flat, heads * LANES), 0)
        == lax.shift_right_logical(col, bits(LANES)) * head_dim + (col & (head_dim - 1)),
        1.0,
        0.0,
    ).astype(BF16)
    own_block = (
        lax.shift_right_logical(iota((grid_rows, seqs * head_dim), 1), bits(head_dim))
        == (iota((grid_rows, seqs * head_dim), 0) & (seqs - 1))
    )
    row = iota((2 * LANES, 2 * LANES), 0) & (LANES - 1)
    column = iota((2 * LANES, 2 * LANES), 1)
    later_table = jnp.where((column >= LANES) | (row > column), 1.0, 0.0).astype(BF16)
    row_seq = iota((grid_rows, 1), 0) & (seqs - 1)
    row_head = lax.shift_right_logical(iota((grid_rows, 1), 0), bits(seqs))
    filled = jnp.zeros((grid_rows, 1), jnp.int32)
    for s in range(seqs):
        filled = jnp.where(row_seq == s, lengths[s], filled)
    row_bias = jnp.zeros((grid_rows, 1), F32)
    for h in range(heads):
        row_bias = jnp.where(row_head == h, bias[h], row_bias)

    loads[3].wait()
    queries = dot(normed, wq_v[...]).astype(BF16)
    twice = dot(queries, spread_table)
    stacked = jnp.concatenate([twice[:, h * LANES : (h + 1) * LANES] for h in range(heads)], axis=0)
    tiled = jnp.concatenate([stacked] * (seqs * head_dim // LANES), axis=1)
    query_grid = jnp.where(own_block, tiled, 0.0).astype(BF16)
    scores = None
    for c in range(chunks):
        key_loads[c].wait()
        part = dot(query_grid[:, c * span : (c + 1) * span], k_v[c * span : (c + 1) * span, :])
        scores = part if scores is None else scores + part
    scores = scores * head_dim ** (-0.5) + row_bias
    visible = iota((grid_rows, length), 1) < filled
    soft = jnp.log1p(jnp.exp(-jnp.abs(scores)))
    log_keep = jnp.where(visible, jnp.minimum(-scores, 0.0) - soft, 0.0)
    log_take = jnp.minimum(scores, 0.0) - soft
    count = length // LANES
    keep_hi = log_keep.astype(BF16).astype(F32)
    keep_lo = log_keep - keep_hi
    stack = jnp.concatenate(
        [
            jnp.concatenate(
                [keep_hi[:, c * LANES : (c + 1) * LANES], keep_lo[:, c * LANES : (c + 1) * LANES]], axis=1
            )
            for c in range(count)
        ],
        axis=0,
    ).astype(BF16)
    sums = dot(stack, later_table)
    carried = jnp.zeros((grid_rows, LANES), F32)
    pieces = [None] * count
    for c in reversed(range(count)):
        here = sums[c * grid_rows : (c + 1) * grid_rows]
        pieces[c] = here[:, :LANES] + carried
        carried = carried + here[:, LANES:]
    later = jnp.concatenate(pieces, axis=1)
    stick = jnp.where(visible, jnp.exp(log_take + later), 0.0).astype(BF16)
    folded = jnp.zeros((grid_rows, LANES), F32)
    for c in range(chunks):
        value_loads[c].wait()
        part = dot_nt(stick, v_v[c * span : (c + 1) * span, :])
        part = jnp.where(own_block[:, c * span : (c + 1) * span], part, 0.0)
        for b in range(span // LANES):
            folded = folded + part[:, b * LANES : (b + 1) * LANES]
    folded = jnp.concatenate([folded[h * seqs : (h + 1) * seqs] for h in range(heads)], axis=1)
    attended = dot_nt(folded.astype(BF16), spread_table).astype(BF16)
    wo_load.wait()
    part_proj = dot(attended, wo_v[...])
    proj_out[...] = part_proj

    def swap(index, source, target):
        return pltpu.make_async_remote_copy(
            src_ref=source,
            dst_ref=target,
            send_sem=ts.at[index],
            recv_sem=tr.at[index],
            device_id=(me, other),
            device_id_type=MESH,
        )

    proj_swap = swap(0, proj_out, proj_in)
    proj_swap.start()
    wk_load.wait()
    fresh_k[...] = dot(normed, wk_v[...]).astype(BF16)
    wv_load.wait()
    fresh_v[...] = dot(normed, wv_v[...]).astype(BF16)
    proj_swap.wait()
    projected = part_proj + proj_in[...]
    hidden = layer_norm(normed.astype(F32) + projected, norm_mid[...]).astype(BF16)

    outgoing[...] = dot_tn(chosen, hidden).astype(BF16)

    def dispatch(p, source, target):
        return pltpu.make_async_remote_copy(
            src_ref=outgoing.at[block(source, slots), :],
            dst_ref=received.at[block(target, slots), :],
            send_sem=ds.at[p],
            recv_sem=dr.at[p],
            device_id=(lax.rem(me + p, ep), core),
            device_id_type=MESH,
        )

    def start_dispatch(p, c):
        dispatch(p, lax.rem(me + p, ep), me).start()
        return c

    lax.fori_loop(1, ep, start_dispatch, 0)
    own_rows = pltpu.make_async_copy(
        outgoing.at[block(me, slots), :], received.at[block(me, slots), :], own_sem.at[1]
    )
    own_rows.start()

    hidden_f = hidden.astype(F32)
    mix_weight = sigmoid(jnp.sum(hidden_f * mix_gate[...], axis=-1, keepdims=True))

    def wait_gather(p, c):
        done = gather(p, lax.rem(me + ep - p, ep))
        done.wait_recv()
        done.wait_send()
        return c

    lax.fori_loop(1, ep, wait_gather, 0)
    own_gather.wait()
    dense_pre = dot(hidden, gath[0])
    dense_lin = dot(hidden, gath[1])
    dense_act = (dense_pre * sigmoid(dense_pre) * dense_lin).astype(BF16)
    dense_part = dot_nt(dense_act, gath[2]) * mix_weight

    eg_load.wait()
    eu_load.wait()
    ed_load.wait()

    def wait_dispatch(p, c):
        source = lax.rem(me + ep - p, ep)
        done = dispatch(p, lax.rem(me + p, ep), source)
        done.wait_recv()
        done.wait_send()
        return c

    lax.fori_loop(1, ep, wait_dispatch, 0)
    own_rows.wait()
    token_rows = received[...]
    gate_pre = dot(token_rows, eg_v[...])
    up_pre = dot(token_rows, eu_v[...])
    act = (gate_pre * sigmoid(gate_pre) * up_pre).astype(BF16)
    expert_y[...] = dot(act, ed_v[...]).astype(BF16)

    def give_back(p, source, target):
        return pltpu.make_async_remote_copy(
            src_ref=expert_y.at[block(source, slots), :],
            dst_ref=returned.at[block(target, slots), :],
            send_sem=rs.at[p],
            recv_sem=rr.at[p],
            device_id=(lax.rem(me + p, ep), core),
            device_id_type=MESH,
        )

    def start_return(p, c):
        give_back(p, lax.rem(me + p, ep), me).start()
        return c

    lax.fori_loop(1, ep, start_return, 0)
    own_back = pltpu.make_async_copy(
        expert_y.at[block(me, slots), :], returned.at[block(me, slots), :], own_sem.at[2]
    )
    own_back.start()

    def wait_return(p, c):
        source = lax.rem(me + ep - p, ep)
        done = give_back(p, lax.rem(me + p, ep), source)
        done.wait_recv()
        done.wait_send()
        return c

    lax.fori_loop(1, ep, wait_return, 0)
    own_back.wait()
    routed3 = dot(weight_split, returned[...])
    routed = routed3[:seqs] + routed3[seqs : 2 * seqs] + routed3[2 * seqs :]
    final = routed + dense_part
    fin_out[...] = final
    fin_swap = swap(1, fin_out, fin_in)
    fin_swap.start()
    fin_swap.wait()
    combined = hidden_f + (final + fin_in[...])
    mixed[...] = layer_norm(combined, norm_out[...]).astype(BF16)


def shards(
    tokens, cache_keys, cache_values, cache_lengths, norm_in, w_query, w_key, w_value, stick_bias,
    w_output, norm_mid, routes, route_weights, expert_gate, expert_up, expert_down,
    dense_gate, dense_up, dense_down, mix_gate, norm_out,
):
    ep = lax.axis_size("ep")
    tp = lax.axis_size("tp")
    seqs, width = tokens.shape
    head_dim, length = cache_keys.shape[2:]
    chunks = 4
    topk = routes.shape[1]
    capacity = max(2, -(-seqs * topk // ep))
    slots = 8
    while slots < capacity:
        slots *= 2
    hidden_units = expert_gate.shape[2]
    rows = dense_gate.shape[0]
    share = dense_gate.shape[1] // tp
    flat_cache = (seqs * head_dim, length)
    total = ep * slots
    vmem = pl.BlockSpec(memory_space=pltpu.VMEM)
    smem = pl.BlockSpec(memory_space=pltpu.SMEM)
    hbm = pl.BlockSpec(memory_space=pl.ANY)
    dma = pltpu.SemaphoreType.DMA
    return pl.pallas_call(
        functools.partial(layer_kernel, ep, slots, chunks, head_dim),
        out_shape=(
            jax.ShapeDtypeStruct((seqs, width), BF16),
            jax.ShapeDtypeStruct((seqs, w_key.shape[1]), BF16),
            jax.ShapeDtypeStruct((seqs, w_value.shape[1]), BF16),
        ),
        in_specs=[vmem] * 7 + [smem] * 2 + [hbm] * 12,
        out_specs=(vmem, vmem, vmem),
        scratch_shapes=[
            pltpu.VMEM(w_query.shape, BF16),
            pltpu.VMEM(w_key.shape, BF16),
            pltpu.VMEM(w_value.shape, BF16),
            pltpu.VMEM(flat_cache, BF16),
            pltpu.VMEM(flat_cache, BF16),
            pltpu.VMEM(w_output.shape, BF16),
            pltpu.VMEM((width, hidden_units), BF16),
            pltpu.VMEM((width, hidden_units), BF16),
            pltpu.VMEM((hidden_units, width), BF16),
            pltpu.VMEM((share, dense_down.shape[1]), BF16),
            pltpu.VMEM((3, rows, share), BF16),
            pltpu.VMEM((3, ep * rows, share), BF16),
            pltpu.VMEM((seqs, width), F32),
            pltpu.VMEM((seqs, width), F32),
            pltpu.VMEM((total, width), BF16),
            pltpu.VMEM((total, width), BF16),
            pltpu.VMEM((total, width), BF16),
            pltpu.VMEM((total, width), BF16),
            pltpu.VMEM((seqs, width), F32),
            pltpu.VMEM((seqs, width), F32),
            dma((10 + 2 * chunks,)),
            dma((3,)),
            dma((ep,)),
            dma((ep,)),
            dma((ep,)),
            dma((ep,)),
            dma((ep,)),
            dma((ep,)),
            dma((2,)),
            dma((2,)),
        ],
        compiler_params=pltpu.CompilerParams(
            collective_id=0, has_side_effects=True, vmem_limit_bytes=60 * 1024 * 1024
        ),
    )(
        tokens,
        norm_in.reshape(1, width),
        norm_mid.reshape(1, width),
        norm_out.reshape(1, width),
        mix_gate.reshape(1, width),
        routes,
        route_weights,
        cache_lengths,
        stick_bias,
        w_query,
        w_key,
        w_value,
        cache_keys.reshape(flat_cache),
        cache_values.reshape(flat_cache),
        w_output,
        expert_gate.reshape(width, hidden_units),
        expert_up.reshape(width, hidden_units),
        expert_down.reshape(hidden_units, width),
        dense_gate,
        dense_up,
        dense_down,
    )


def solution(mesh):
    in_specs = (
        P("ep", None),
        P("ep", "tp", None, None),
        P("ep", "tp", None, None),
        P("ep"),
        P(),
        P(None, "tp"),
        P(None, "tp"),
        P(None, "tp"),
        P("tp"),
        P("tp", None),
        P(),
        P("ep", None),
        P("ep", None),
        P("ep", None, "tp"),
        P("ep", None, "tp"),
        P("ep", "tp", None),
        P("ep", None),
        P("ep", None),
        P(None, "ep"),
        P(),
        P(),
    )
    out_specs = (P("ep", None), P("ep", "tp"), P("ep", "tp"))
    return jax.shard_map(shards, mesh=mesh, in_specs=in_specs, out_specs=out_specs, check_vma=False)
```

```python
import functools

import jax
import jax.numpy as jnp
from jax import lax
from jax.experimental import pallas as pl
from jax.experimental.pallas import tpu as pltpu
from jax.sharding import PartitionSpec as P

MESH = pl.DeviceIdType.MESH
F32 = jnp.float32
BF16 = jnp.bfloat16
LANES = 128


def layer_norm(values, gain):
    center = jnp.mean(values, -1, keepdims=True)
    spread = jnp.mean(jnp.square(values - center), -1, keepdims=True)
    return (values - center) * lax.rsqrt(spread + 1e-05) * gain


def sigmoid(x):
    return 1.0 / (1.0 + jnp.exp(-x))


def iota(shape, dim):
    return lax.broadcasted_iota(jnp.int32, shape, dim)


def bits(n):
    assert n & (n - 1) == 0
    return n.bit_length() - 1


def dot(a, b):
    return jnp.dot(a, b, preferred_element_type=F32)


def dot_nt(a, b):
    return lax.dot_general(a, b, (((1,), (1,)), ((), ())), preferred_element_type=F32)


def dot_tn(a, b):
    return lax.dot_general(a, b, (((0,), (0,)), ((), ())), preferred_element_type=F32)


def layer_kernel(
    ep, slots, chunks, head_dim,
    tokens, norm_in, norm_mid, norm_out, mix_gate, routes, route_weights, lengths, bias,
    wq, wk, wv, keys, values, wo, eg, eu, ed, dg, du, dd,
    mixed, fresh_k, fresh_v,
    wq_v, wk_v, wv_v, k_v, v_v, wo_v, eg_v, eu_v, ed_v, dd_v,
    pack, gath, proj_out, proj_in, hid_v, outgoing, received, received_other, part_out, part_in,
    expert_y, returned, fin_out, fin_in, mixed_v, fresh_k_v, fresh_v_v,
    load_sem, own_sem, out_sem, gs, gr, ds, dr, rs, rr, ts, tr,
):
    me = lax.axis_index("ep")
    core = lax.axis_index("tp")
    other = 1 - core
    seqs, width = tokens.shape
    heads = bias.shape[0]
    length = keys.shape[1]
    rows = dg.shape[0]
    share = pack.shape[2]

    barrier = pltpu.get_barrier_semaphore()

    half = width // 2
    mine = pl.ds(pl.multiple_of(core * half, half), half)
    theirs = pl.ds(pl.multiple_of(other * half, half), half)

    def greet(p, c):
        pl.semaphore_signal(
            barrier, inc=1, device_id=(lax.rem(me + p, ep), core), device_id_type=MESH
        )
        return c

    lax.fori_loop(1, ep, greet, 0)
    pl.semaphore_signal(barrier, inc=1, device_id=(me, other), device_id_type=MESH)

    offset = pl.multiple_of(core * share, share)
    span = keys.shape[0] // chunks
    moves = [
        (dd.at[pl.ds(offset, share), :], dd_v),
        (dg.at[:, pl.ds(offset, share)], pack.at[0]),
        (du.at[:, pl.ds(offset, share)], pack.at[1]),
        (wq, wq_v),
    ]
    moves += [(keys.at[pl.ds(c * span, span)], k_v.at[pl.ds(c * span, span)]) for c in range(chunks)]
    moves += [(values.at[pl.ds(c * span, span)], v_v.at[pl.ds(c * span, span)]) for c in range(chunks)]
    moves += [(wo, wo_v), (wk, wk_v), (wv, wv_v), (eg, eg_v), (eu, eu_v), (ed, ed_v)]
    loads = [pltpu.make_async_copy(a, b, load_sem.at[i]) for i, (a, b) in enumerate(moves)]
    for load in loads:
        load.start()
    key_loads = loads[4 : 4 + chunks]
    value_loads = loads[4 + chunks : 4 + 2 * chunks]
    wo_load, wk_load, wv_load, eg_load, eu_load, ed_load = loads[4 + 2 * chunks :]

    normed = layer_norm(tokens[...].astype(F32), norm_in[...]).astype(BF16)

    for load in loads[:3]:
        load.wait()
    pack[2] = dd_v[...].astype(F32).T.astype(BF16)

    def block(index, size):
        return pl.ds(pl.multiple_of(index * size, size), size)

    pl.semaphore_wait(barrier, ep)

    levels = bits(ep)
    my_bits = [lax.rem(me // (1 << k), 2) for k in range(levels)]

    def flip(mask):
        index = me
        for k in range(levels):
            if mask >> k & 1:
                index = index + (1 - 2 * my_bits[k]) * (1 << k)
        return index

    down = list(reversed(range(levels)))
    orders = [down, down[:-2] + [0, 1], [0, 1] + down[:-2]]
    steps = [[] for _ in range(levels)]
    number = 0
    for array, order in enumerate(orders):
        held = [0]
        for step, bit in enumerate(order):
            for mask in held:
                steps[step].append((number, array, mask, mask | 1 << bit, 1 << bit))
                number += 1
            held = held + [mask | 1 << bit for mask in held]

    def gather(item, incoming):
        number, array, mask, far_mask, bit = item
        return pltpu.make_async_remote_copy(
            src_ref=gath.at[array, block(flip(mask), rows), :] if mask else pack.at[array],
            dst_ref=gath.at[array, block(flip(far_mask if incoming else mask), rows), :],
            send_sem=gs.at[number],
            recv_sem=gr.at[number],
            device_id=(flip(bit), core),
            device_id_type=MESH,
        )

    def gather_start(step):
        for item in steps[step]:
            gather(item, False).start()

    def gather_wait(step):
        for item in steps[step]:
            gather(item, True).wait_recv()

    gather_start(0)
    own_gather = pltpu.make_async_copy(pack, gath.at[:, block(me, rows), :], own_sem.at[0])
    own_gather.start()

    total = ep * slots
    slot_of = iota((total, seqs), 0)
    expert_of = lax.shift_right_logical(slot_of, bits(slots))
    place_of = slot_of & (slots - 1)
    route_rows = routes[...]
    weight_rows = route_weights[...]
    member = jnp.zeros((total, seqs), F32)
    weight = jnp.zeros((total, seqs), F32)
    for k in range(route_rows.shape[0]):
        hit = route_rows[k : k + 1, :] == expert_of
        member = jnp.where(hit, 1.0, member)
        weight = jnp.where(hit, weight_rows[k : k + 1, :], weight)
    earlier = jnp.where(iota((seqs, seqs), 0) < iota((seqs, seqs), 1), 1.0, 0.0).astype(BF16)
    before = dot(member.astype(BF16), earlier).astype(jnp.int32)
    chosen = jnp.where(before == place_of, member, 0.0)
    weight = (weight * chosen).T
    chosen = chosen.astype(BF16)
    w_hi = weight.astype(BF16)
    w_rest = weight - w_hi.astype(F32)
    w_mid = w_rest.astype(BF16)
    w_lo = (w_rest - w_mid.astype(F32)).astype(BF16)
    weight_split = jnp.concatenate([w_hi, w_mid, w_lo], axis=0)

    grid_rows = heads * seqs
    flat = heads * head_dim
    col = iota((flat, heads * LANES), 1)
    spread_table = jnp.where(
        iota((flat, heads * LANES), 0)
        == lax.shift_right_logical(col, bits(LANES)) * head_dim + (col & (head_dim - 1)),
        1.0,
        0.0,
    ).astype(BF16)
    own_block = (
        lax.shift_right_logical(iota((grid_rows, seqs * head_dim), 1), bits(head_dim))
        == (iota((grid_rows, seqs * head_dim), 0) & (seqs - 1))
    )
    row = iota((2 * LANES, 2 * LANES), 0) & (LANES - 1)
    column = iota((2 * LANES, 2 * LANES), 1)
    later_table = jnp.where((column >= LANES) | (row > column), 1.0, 0.0).astype(BF16)
    row_seq = iota((grid_rows, 1), 0) & (seqs - 1)
    row_head = lax.shift_right_logical(iota((grid_rows, 1), 0), bits(seqs))
    filled = jnp.zeros((grid_rows, 1), jnp.int32)
    for s in range(seqs):
        filled = jnp.where(row_seq == s, lengths[s], filled)
    row_bias = jnp.zeros((grid_rows, 1), F32)
    for h in range(heads):
        row_bias = jnp.where(row_head == h, bias[h], row_bias)

    loads[3].wait()
    queries = dot(normed, wq_v[...]).astype(BF16)
    twice = dot(queries, spread_table)
    stacked = jnp.concatenate([twice[:, h * LANES : (h + 1) * LANES] for h in range(heads)], axis=0)
    tiled = jnp.concatenate([stacked] * (seqs * head_dim // LANES), axis=1)
    query_grid = jnp.where(own_block, tiled, 0.0).astype(BF16)
    scores = None
    for c in range(chunks):
        key_loads[c].wait()
        part = dot(query_grid[:, c * span : (c + 1) * span], k_v[c * span : (c + 1) * span, :])
        scores = part if scores is None else scores + part
    gather_wait(0)
    gather_start(1)
    scores = scores * head_dim ** (-0.5) + row_bias
    visible = iota((grid_rows, length), 1) < filled
    soft = jnp.log1p(jnp.exp(-jnp.abs(scores)))
    log_keep = jnp.where(visible, jnp.minimum(-scores, 0.0) - soft, 0.0)
    log_take = jnp.minimum(scores, 0.0) - soft
    count = length // LANES
    keep_hi = log_keep.astype(BF16).astype(F32)
    keep_lo = log_keep - keep_hi
    stack = jnp.concatenate(
        [
            jnp.concatenate(
                [keep_hi[:, c * LANES : (c + 1) * LANES], keep_lo[:, c * LANES : (c + 1) * LANES]], axis=1
            )
            for c in range(count)
        ],
        axis=0,
    ).astype(BF16)
    sums = dot(stack, later_table)
    carried = jnp.zeros((grid_rows, LANES), F32)
    pieces = [None] * count
    for c in reversed(range(count)):
        here = sums[c * grid_rows : (c + 1) * grid_rows]
        pieces[c] = here[:, :LANES] + carried
        carried = carried + here[:, LANES:]
    later = jnp.concatenate(pieces, axis=1)
    stick = jnp.where(visible, jnp.exp(log_take + later), 0.0).astype(BF16)
    if levels > 2:
        gather_wait(1)
        gather_start(2)
    folded = jnp.zeros((grid_rows, LANES), F32)
    for c in range(chunks):
        value_loads[c].wait()
        part = dot_nt(stick, v_v[c * span : (c + 1) * span, :])
        part = jnp.where(own_block[:, c * span : (c + 1) * span], part, 0.0)
        for b in range(span // LANES):
            folded = folded + part[:, b * LANES : (b + 1) * LANES]
    folded = jnp.concatenate([folded[h * seqs : (h + 1) * seqs] for h in range(heads)], axis=1)
    attended = dot_nt(folded.astype(BF16), spread_table).astype(BF16)
    wo_load.wait()
    part_proj = dot(attended, wo_v[...])
    proj_out[...] = part_proj

    def swap(index, source, target):
        return pltpu.make_async_remote_copy(
            src_ref=source,
            dst_ref=target,
            send_sem=ts.at[index],
            recv_sem=tr.at[index],
            device_id=(me, other),
            device_id_type=MESH,
        )

    proj_swap = swap(0, proj_out, proj_in)
    proj_swap.start()
    for step in range(3, levels):
        gather_wait(step - 1)
        gather_start(step)
    wk_load.wait()
    fresh_k_v[...] = dot_nt(normed, wk_v[...]).astype(BF16)
    wv_load.wait()
    fresh_v_v[...] = dot_nt(normed, wv_v[...]).astype(BF16)
    fresh_out = [
        pltpu.make_async_copy(fresh_k_v, fresh_k, out_sem.at[0]),
        pltpu.make_async_copy(fresh_v_v, fresh_v, out_sem.at[1]),
    ]
    for copy in fresh_out:
        copy.start()
    proj_swap.wait()
    projected = part_proj + proj_in[...]
    hidden = layer_norm(normed.astype(F32) + projected, norm_mid[...]).astype(BF16)

    hid_v[...] = hidden
    outgoing[...] = dot(chosen, hid_v[:, mine]).astype(BF16)

    def dispatch(p, source, target):
        return pltpu.make_async_remote_copy(
            src_ref=outgoing.at[block(source, slots), :],
            dst_ref=received.at[block(target, slots), :],
            send_sem=ds.at[p],
            recv_sem=dr.at[p],
            device_id=(lax.rem(me + p, ep), core),
            device_id_type=MESH,
        )

    def start_dispatch(p, c):
        dispatch(p, lax.rem(me + p, ep), me).start()
        return c

    lax.fori_loop(1, ep, start_dispatch, 0)
    own_rows = pltpu.make_async_copy(
        outgoing.at[block(me, slots), :], received.at[block(me, slots), :], own_sem.at[1]
    )
    own_rows.start()

    hidden_f = hidden.astype(F32)
    mix_weight = sigmoid(jnp.sum(hidden_f * mix_gate[...], axis=-1, keepdims=True))

    gather_wait(levels - 1)
    for step in range(levels):
        for item in steps[step]:
            gather(item, False).wait_send()
    own_gather.wait()
    dense_pre = dot(hidden, gath[0])
    dense_lin = dot(hidden, gath[1])
    dense_act = (dense_pre * sigmoid(dense_pre) * dense_lin).astype(BF16)
    dense_part = dot_nt(dense_act, gath[2]) * mix_weight

    eg_load.wait()
    eu_load.wait()
    ed_load.wait()

    def wait_dispatch(p, c):
        source = lax.rem(me + ep - p, ep)
        done = dispatch(p, lax.rem(me + p, ep), source)
        done.wait_recv()
        done.wait_send()
        return c

    lax.fori_loop(1, ep, wait_dispatch, 0)
    own_rows.wait()
    row_swap = swap(2, received, received_other)
    row_swap.start()
    near = received[...]
    gate_pre = dot(near, eg_v[mine, :])
    up_pre = dot(near, eu_v[mine, :])
    row_swap.wait()
    far = received_other[...]
    gate_pre = gate_pre + dot(far, eg_v[theirs, :])
    up_pre = up_pre + dot(far, eu_v[theirs, :])
    act = (gate_pre * sigmoid(gate_pre) * up_pre).astype(BF16)
    part_out[...] = dot(act, ed_v[:, theirs]).astype(BF16)
    part_swap = swap(3, part_out, part_in)
    part_swap.start()
    own_part = dot(act, ed_v[:, mine]).astype(BF16).astype(F32)
    part_swap.wait()
    expert_y[...] = (own_part + part_in[...].astype(F32)).astype(BF16)

    def give_back(p, source, target):
        return pltpu.make_async_remote_copy(
            src_ref=expert_y.at[block(source, slots), :],
            dst_ref=returned.at[block(target, slots), :],
            send_sem=rs.at[p],
            recv_sem=rr.at[p],
            device_id=(lax.rem(me + p, ep), core),
            device_id_type=MESH,
        )

    def start_return(p, c):
        give_back(p, lax.rem(me + p, ep), me).start()
        return c

    lax.fori_loop(1, ep, start_return, 0)
    own_back = pltpu.make_async_copy(
        expert_y.at[block(me, slots), :], returned.at[block(me, slots), :], own_sem.at[2]
    )
    own_back.start()

    def wait_return(p, c):
        source = lax.rem(me + ep - p, ep)
        done = give_back(p, lax.rem(me + p, ep), source)
        done.wait_recv()
        done.wait_send()
        return c

    lax.fori_loop(1, ep, wait_return, 0)
    own_back.wait()
    routed3 = dot(weight_split, returned[...])
    routed = routed3[:seqs] + routed3[seqs : 2 * seqs] + routed3[2 * seqs :]
    fin_out[...] = dense_part
    fin_out[:, mine] = fin_out[:, mine] + routed
    fin_swap = swap(1, fin_out, fin_in)
    fin_swap.start()
    for copy in fresh_out:
        copy.wait()
    fin_swap.wait()
    combined = hidden_f + (fin_out[...] + fin_in[...])
    mixed_v[...] = layer_norm(combined, norm_out[...]).astype(BF16)
    result = pltpu.make_async_copy(mixed_v, mixed, out_sem.at[2])
    result.start()
    result.wait()


def shards(
    tokens, cache_keys, cache_values, cache_lengths, norm_in, w_query, w_key, w_value, stick_bias,
    w_output, norm_mid, routes, route_weights, expert_gate, expert_up, expert_down,
    dense_gate, dense_up, dense_down, mix_gate, norm_out,
):
    ep = lax.axis_size("ep")
    tp = lax.axis_size("tp")
    seqs, width = tokens.shape
    head_dim, length = cache_keys.shape[2:]
    chunks = 4
    topk = routes.shape[1]
    capacity = max(2, -(-seqs * topk // ep))
    slots = 8
    while slots < capacity:
        slots *= 2
    hidden_units = expert_gate.shape[2]
    rows = dense_gate.shape[0]
    share = dense_gate.shape[1] // tp
    flat_cache = (seqs * head_dim, length)
    total = ep * slots
    vmem = pl.BlockSpec(memory_space=pltpu.VMEM)
    smem = pl.BlockSpec(memory_space=pltpu.SMEM)
    hbm = pl.BlockSpec(memory_space=pl.ANY)
    hbm_out = pl.BlockSpec(memory_space=pltpu.HBM)
    half = width // 2
    dma = pltpu.SemaphoreType.DMA
    return pl.pallas_call(
        functools.partial(layer_kernel, ep, slots, chunks, head_dim),
        out_shape=(
            jax.ShapeDtypeStruct((seqs, width), BF16),
            jax.ShapeDtypeStruct((seqs, w_key.shape[1]), BF16),
            jax.ShapeDtypeStruct((seqs, w_value.shape[1]), BF16),
        ),
        in_specs=[vmem] * 7 + [smem] * 2 + [hbm] * 12,
        out_specs=(hbm_out, hbm_out, hbm_out),
        scratch_shapes=[
            pltpu.VMEM(w_query.shape, BF16),
            pltpu.VMEM(w_key.shape[::-1], BF16),
            pltpu.VMEM(w_value.shape[::-1], BF16),
            pltpu.VMEM(flat_cache, BF16),
            pltpu.VMEM(flat_cache, BF16),
            pltpu.VMEM(w_output.shape, BF16),
            pltpu.VMEM((width, hidden_units), BF16),
            pltpu.VMEM((width, hidden_units), BF16),
            pltpu.VMEM((hidden_units, width), BF16),
            pltpu.VMEM((share, dense_down.shape[1]), BF16),
            pltpu.VMEM((3, rows, share), BF16),
            pltpu.VMEM((3, ep * rows, share), BF16),
            pltpu.VMEM((seqs, width), F32),
            pltpu.VMEM((seqs, width), F32),
            pltpu.VMEM((seqs, width), BF16),
            *[pltpu.VMEM((total, half), BF16)] * 7,
            pltpu.VMEM((seqs, width), F32),
            pltpu.VMEM((seqs, width), F32),
            pltpu.VMEM((seqs, width), BF16),
            pltpu.VMEM((seqs, w_key.shape[1]), BF16),
            pltpu.VMEM((seqs, w_value.shape[1]), BF16),
            dma((10 + 2 * chunks,)),
            dma((3,)),
            dma((3,)),
            dma((3 * ep,)),
            dma((3 * ep,)),
            dma((ep,)),
            dma((ep,)),
            dma((ep,)),
            dma((ep,)),
            dma((4,)),
            dma((4,)),
        ],
        compiler_params=pltpu.CompilerParams(
            collective_id=0, has_side_effects=True, vmem_limit_bytes=60 * 1024 * 1024
        ),
    )(
        tokens,
        norm_in.reshape(1, width),
        norm_mid.reshape(1, width),
        norm_out.reshape(1, width),
        mix_gate.reshape(1, width),
        routes.T,
        route_weights.T,
        cache_lengths,
        stick_bias,
        w_query,
        w_key.T,
        w_value.T,
        cache_keys.reshape(flat_cache),
        cache_values.reshape(flat_cache),
        w_output,
        expert_gate.reshape(width, hidden_units),
        expert_up.reshape(width, hidden_units),
        expert_down.reshape(hidden_units, width),
        dense_gate,
        dense_up,
        dense_down,
    )


def solution(mesh):
    in_specs = (
        P("ep", None),
        P("ep", "tp", None, None),
        P("ep", "tp", None, None),
        P("ep"),
        P(),
        P(None, "tp"),
        P(None, "tp"),
        P(None, "tp"),
        P("tp"),
        P("tp", None),
        P(),
        P("ep", None),
        P("ep", None),
        P("ep", None, "tp"),
        P("ep", None, "tp"),
        P("ep", "tp", None),
        P("ep", None),
        P("ep", None),
        P(None, "ep"),
        P(),
        P(),
    )
    out_specs = (P("ep", None), P("ep", "tp"), P("ep", "tp"))
    return jax.shard_map(shards, mesh=mesh, in_specs=in_specs, out_specs=out_specs, check_vma=False)
```

```python
import functools

import jax
import jax.numpy as jnp
from jax import lax
from jax.experimental import pallas as pl
from jax.experimental.pallas import tpu as pltpu
from jax.sharding import PartitionSpec as P

MESH = pl.DeviceIdType.MESH
F32 = jnp.float32
BF16 = jnp.bfloat16
LANES = 128
PLAN = (3, 4, 5)


def layer_norm(values, gain):
    center = jnp.mean(values, -1, keepdims=True)
    spread = jnp.mean(jnp.square(values - center), -1, keepdims=True)
    return (values - center) * lax.rsqrt(spread + 1e-05) * gain


def sigmoid(x):
    return 1.0 / (1.0 + jnp.exp(-x))


def iota(shape, dim):
    return lax.broadcasted_iota(jnp.int32, shape, dim)


def bits(n):
    assert n & (n - 1) == 0
    return n.bit_length() - 1


def dot(a, b):
    return jnp.dot(a, b, preferred_element_type=F32)


def dot_nt(a, b):
    return lax.dot_general(a, b, (((1,), (1,)), ((), ())), preferred_element_type=F32)


def dot_tn(a, b):
    return lax.dot_general(a, b, (((0,), (0,)), ((), ())), preferred_element_type=F32)


def layer_kernel(
    ep, slots, chunks, head_dim,
    tokens, norm_in, norm_mid, mix_gate, routes, route_weights, lengths, bias,
    wq, wk, wv, keys, values, wo, eg, eu, ed, dg, du, dd,
    combined, fresh_k, fresh_v,
    wq_v, wk_v, wv_v, k_v, v_v, wo_v, eg_v, eu_v, ed_v, dd_v,
    pack, gath, proj_out, proj_in, hid_v, outgoing, received, received_other, part_out, part_in,
    expert_y, returned, fin_out, fin_in,
    load_sem, own_sem, gs, gr, ds, dr, rs, rr, ts, tr,
):
    me = lax.axis_index("ep")
    core = lax.axis_index("tp")
    other = 1 - core
    seqs, width = tokens.shape
    heads = bias.shape[0]
    length = keys.shape[1]
    rows = dg.shape[0]
    share = pack.shape[2]

    barrier = pltpu.get_barrier_semaphore()

    half = width // 2
    mine = pl.ds(pl.multiple_of(core * half, half), half)
    theirs = pl.ds(pl.multiple_of(other * half, half), half)

    def greet(p, c):
        pl.semaphore_signal(
            barrier, inc=1, device_id=(lax.rem(me + p, ep), core), device_id_type=MESH
        )
        return c

    lax.fori_loop(1, ep, greet, 0)
    pl.semaphore_signal(barrier, inc=1, device_id=(me, other), device_id_type=MESH)

    offset = pl.multiple_of(core * share, share)
    span = keys.shape[0] // chunks
    moves = [
        (dd.at[pl.ds(offset, share), :], dd_v),
        (dg.at[:, pl.ds(offset, share)], pack.at[0]),
        (du.at[:, pl.ds(offset, share)], pack.at[1]),
        (wq, wq_v),
    ]
    moves += [(keys.at[pl.ds(c * span, span)], k_v.at[pl.ds(c * span, span)]) for c in range(chunks)]
    moves += [(values.at[pl.ds(c * span, span)], v_v.at[pl.ds(c * span, span)]) for c in range(chunks)]
    moves += [(wo, wo_v), (wk, wk_v), (wv, wv_v), (eg, eg_v), (eu, eu_v), (ed, ed_v)]
    loads = [pltpu.make_async_copy(a, b, load_sem.at[i]) for i, (a, b) in enumerate(moves)]
    for load in loads:
        load.start()
    key_loads = loads[4 : 4 + chunks]
    value_loads = loads[4 + chunks : 4 + 2 * chunks]
    wo_load, wk_load, wv_load, eg_load, eu_load, ed_load = loads[4 + 2 * chunks :]

    normed = layer_norm(tokens[...].astype(F32), norm_in[...]).astype(BF16)

    total = ep * slots
    slot_of = iota((total, seqs), 0)
    expert_of = lax.shift_right_logical(slot_of, bits(slots))
    place_of = slot_of & (slots - 1)
    route_rows = routes[...]
    weight_rows = route_weights[...]
    member = jnp.zeros((total, seqs), F32)
    weight = jnp.zeros((total, seqs), F32)
    for k in range(route_rows.shape[0]):
        hit = route_rows[k : k + 1, :] == expert_of
        member = jnp.where(hit, 1.0, member)
        weight = jnp.where(hit, weight_rows[k : k + 1, :], weight)
    earlier = jnp.where(iota((seqs, seqs), 0) < iota((seqs, seqs), 1), 1.0, 0.0).astype(BF16)
    before = dot(member.astype(BF16), earlier).astype(jnp.int32)
    chosen = jnp.where(before == place_of, member, 0.0)
    weight = (weight * chosen).T
    chosen = chosen.astype(BF16)
    w_hi = weight.astype(BF16)
    w_rest = weight - w_hi.astype(F32)
    w_mid = w_rest.astype(BF16)
    w_lo = (w_rest - w_mid.astype(F32)).astype(BF16)
    weight_split = jnp.concatenate([w_hi, w_mid, w_lo], axis=0)

    grid_rows = heads * seqs
    flat = heads * head_dim
    col = iota((flat, heads * LANES), 1)
    spread_table = jnp.where(
        iota((flat, heads * LANES), 0)
        == lax.shift_right_logical(col, bits(LANES)) * head_dim + (col & (head_dim - 1)),
        1.0,
        0.0,
    ).astype(BF16)
    own_block = (
        lax.shift_right_logical(iota((grid_rows, seqs * head_dim), 1), bits(head_dim))
        == (iota((grid_rows, seqs * head_dim), 0) & (seqs - 1))
    )
    row = iota((2 * LANES, 2 * LANES), 0) & (LANES - 1)
    column = iota((2 * LANES, 2 * LANES), 1)
    later_table = jnp.where((column >= LANES) | (row > column), 1.0, 0.0).astype(BF16)
    row_seq = iota((grid_rows, 1), 0) & (seqs - 1)
    row_head = lax.shift_right_logical(iota((grid_rows, 1), 0), bits(seqs))
    filled = jnp.zeros((grid_rows, 1), jnp.int32)
    for s in range(seqs):
        filled = jnp.where(row_seq == s, lengths[s], filled)
    row_bias = jnp.zeros((grid_rows, 1), F32)
    for h in range(heads):
        row_bias = jnp.where(row_head == h, bias[h], row_bias)

    for load in loads[:3]:
        load.wait()
    pack[2] = dd_v[...].astype(F32).T.astype(BF16)

    def block(index, size):
        return pl.ds(pl.multiple_of(index * size, size), size)

    pl.semaphore_wait(barrier, ep)

    levels = bits(ep)
    my_bits = [lax.rem(me // (1 << k), 2) for k in range(levels)]

    def flip(mask):
        index = me
        for k in range(levels):
            if mask >> k & 1:
                index = index + (1 - 2 * my_bits[k]) * (1 << k)
        return index

    down = list(reversed(range(levels)))
    orders = [down, down[:-2] + [0, 1], [0, 1] + down[:-2]]
    steps = [[] for _ in range(levels)]
    number = 0
    for array, order in enumerate(orders):
        held = [0]
        for step, bit in enumerate(order):
            for mask in held:
                steps[step].append((number, array, mask, mask | 1 << bit, 1 << bit))
                number += 1
            held = held + [mask | 1 << bit for mask in held]

    def gather(item, incoming):
        number, array, mask, far_mask, bit = item
        return pltpu.make_async_remote_copy(
            src_ref=gath.at[array, block(flip(mask), rows), :] if mask else pack.at[array],
            dst_ref=gath.at[array, block(flip(far_mask if incoming else mask), rows), :],
            send_sem=gs.at[number],
            recv_sem=gr.at[number],
            device_id=(flip(bit), core),
            device_id_type=MESH,
        )

    def gather_start(step):
        for item in steps[step]:
            gather(item, False).start()

    def gather_wait(step):
        for item in steps[step]:
            gather(item, True).wait_recv()

    def advance(point):
        for step in range(1, levels):
            if PLAN[min(step - 1, len(PLAN) - 1)] == point:
                gather_wait(step - 1)
                gather_start(step)

    gather_start(0)
    own_gather = pltpu.make_async_copy(pack, gath.at[:, block(me, rows), :], own_sem.at[0])
    own_gather.start()

    loads[3].wait()
    queries = dot(normed, wq_v[...]).astype(BF16)
    twice = dot(queries, spread_table)
    stacked = jnp.concatenate([twice[:, h * LANES : (h + 1) * LANES] for h in range(heads)], axis=0)
    tiled = jnp.concatenate([stacked] * (seqs * head_dim // LANES), axis=1)
    query_grid = jnp.where(own_block, tiled, 0.0).astype(BF16)
    scores = None
    for c in range(chunks):
        key_loads[c].wait()
        part = dot(query_grid[:, c * span : (c + 1) * span], k_v[c * span : (c + 1) * span, :])
        scores = part if scores is None else scores + part
    advance(1)
    scores = scores * head_dim ** (-0.5) + row_bias
    visible = iota((grid_rows, length), 1) < filled
    soft = jnp.log1p(jnp.exp(-jnp.abs(scores)))
    log_keep = jnp.where(visible, jnp.minimum(-scores, 0.0) - soft, 0.0)
    log_take = jnp.minimum(scores, 0.0) - soft
    count = length // LANES
    keep_hi = log_keep.astype(BF16).astype(F32)
    keep_lo = log_keep - keep_hi
    stack = jnp.concatenate(
        [
            jnp.concatenate(
                [keep_hi[:, c * LANES : (c + 1) * LANES], keep_lo[:, c * LANES : (c + 1) * LANES]], axis=1
            )
            for c in range(count)
        ],
        axis=0,
    ).astype(BF16)
    sums = dot(stack, later_table)
    carried = jnp.zeros((grid_rows, LANES), F32)
    pieces = [None] * count
    for c in reversed(range(count)):
        here = sums[c * grid_rows : (c + 1) * grid_rows]
        pieces[c] = here[:, :LANES] + carried
        carried = carried + here[:, LANES:]
    later = jnp.concatenate(pieces, axis=1)
    stick = jnp.where(visible, jnp.exp(log_take + later), 0.0).astype(BF16)
    advance(2)
    folded = jnp.zeros((grid_rows, LANES), F32)
    for c in range(chunks):
        value_loads[c].wait()
        part = dot_nt(stick, v_v[c * span : (c + 1) * span, :])
        part = jnp.where(own_block[:, c * span : (c + 1) * span], part, 0.0)
        for b in range(span // LANES):
            folded = folded + part[:, b * LANES : (b + 1) * LANES]
    folded = jnp.concatenate([folded[h * seqs : (h + 1) * seqs] for h in range(heads)], axis=1)
    attended = dot_nt(folded.astype(BF16), spread_table).astype(BF16)
    wo_load.wait()
    part_proj = dot(attended, wo_v[...])
    proj_out[...] = part_proj

    def swap(index, source, target):
        return pltpu.make_async_remote_copy(
            src_ref=source,
            dst_ref=target,
            send_sem=ts.at[index],
            recv_sem=tr.at[index],
            device_id=(me, other),
            device_id_type=MESH,
        )

    proj_swap = swap(0, proj_out, proj_in)
    proj_swap.start()
    advance(3)
    wk_load.wait()
    fresh_k[...] = dot_nt(normed, wk_v[...]).astype(BF16)
    wv_load.wait()
    fresh_v[...] = dot_nt(normed, wv_v[...]).astype(BF16)
    proj_swap.wait()
    projected = part_proj + proj_in[...]
    hidden = layer_norm(normed.astype(F32) + projected, norm_mid[...]).astype(BF16)

    hid_v[...] = hidden
    outgoing[...] = dot(chosen, hid_v[:, mine]).astype(BF16)

    def dispatch(p, source, target):
        return pltpu.make_async_remote_copy(
            src_ref=outgoing.at[block(source, slots), :],
            dst_ref=received.at[block(target, slots), :],
            send_sem=ds.at[p],
            recv_sem=dr.at[p],
            device_id=(lax.rem(me + p, ep), core),
            device_id_type=MESH,
        )

    def start_dispatch(p, c):
        dispatch(p, lax.rem(me + p, ep), me).start()
        return c

    lax.fori_loop(1, ep, start_dispatch, 0)
    own_rows = pltpu.make_async_copy(
        outgoing.at[block(me, slots), :], received.at[block(me, slots), :], own_sem.at[1]
    )
    own_rows.start()

    hidden_f = hidden.astype(F32)
    mix_weight = sigmoid(jnp.sum(hidden_f * mix_gate[...], axis=-1, keepdims=True))

    advance(4)

    eg_load.wait()
    eu_load.wait()
    ed_load.wait()

    def wait_dispatch(p, c):
        source = lax.rem(me + ep - p, ep)
        done = dispatch(p, lax.rem(me + p, ep), source)
        done.wait_recv()
        done.wait_send()
        return c

    lax.fori_loop(1, ep, wait_dispatch, 0)
    own_rows.wait()
    row_swap = swap(2, received, received_other)
    row_swap.start()
    advance(5)
    near = received[...]
    gate_pre = dot(near, eg_v[mine, :])
    up_pre = dot(near, eu_v[mine, :])
    row_swap.wait()
    far = received_other[...]
    gate_pre = gate_pre + dot(far, eg_v[theirs, :])
    up_pre = up_pre + dot(far, eu_v[theirs, :])
    act = (gate_pre * sigmoid(gate_pre) * up_pre).astype(BF16)
    part_out[...] = dot(act, ed_v[:, theirs]).astype(BF16)
    part_swap = swap(3, part_out, part_in)
    part_swap.start()
    advance(6)
    own_part = dot(act, ed_v[:, mine]).astype(BF16).astype(F32)
    part_swap.wait()
    expert_y[...] = (own_part + part_in[...].astype(F32)).astype(BF16)

    def give_back(p, source, target):
        return pltpu.make_async_remote_copy(
            src_ref=expert_y.at[block(source, slots), :],
            dst_ref=returned.at[block(target, slots), :],
            send_sem=rs.at[p],
            recv_sem=rr.at[p],
            device_id=(lax.rem(me + p, ep), core),
            device_id_type=MESH,
        )

    def start_return(p, c):
        give_back(p, lax.rem(me + p, ep), me).start()
        return c

    lax.fori_loop(1, ep, start_return, 0)
    own_back = pltpu.make_async_copy(
        expert_y.at[block(me, slots), :], returned.at[block(me, slots), :], own_sem.at[2]
    )
    own_back.start()
    advance(7)
    gather_wait(levels - 1)
    for step in range(levels):
        for item in steps[step]:
            gather(item, False).wait_send()
    own_gather.wait()
    dense_pre = dot(hidden, gath[0])
    dense_lin = dot(hidden, gath[1])
    dense_act = (dense_pre * sigmoid(dense_pre) * dense_lin).astype(BF16)
    dense_part = dot_nt(dense_act, gath[2]) * mix_weight


    def wait_return(p, c):
        source = lax.rem(me + ep - p, ep)
        done = give_back(p, lax.rem(me + p, ep), source)
        done.wait_recv()
        done.wait_send()
        return c

    lax.fori_loop(1, ep, wait_return, 0)
    own_back.wait()
    routed3 = dot(weight_split, returned[...])
    routed = routed3[:seqs] + routed3[seqs : 2 * seqs] + routed3[2 * seqs :]
    fin_out[...] = dense_part
    fin_out[:, mine] = fin_out[:, mine] + routed
    fin_swap = swap(1, fin_out, fin_in)
    fin_swap.start()
    fin_swap.wait()
    combined[...] = hidden_f + (fin_out[...] + fin_in[...])


def finish_kernel(combined, norm_out, fresh_k, fresh_v, mixed, out_k, out_v):
    mixed[...] = layer_norm(combined[...], norm_out[...]).astype(BF16)
    out_k[...] = fresh_k[...]
    out_v[...] = fresh_v[...]


def shards(
    tokens, cache_keys, cache_values, cache_lengths, norm_in, w_query, w_key, w_value, stick_bias,
    w_output, norm_mid, routes, route_weights, expert_gate, expert_up, expert_down,
    dense_gate, dense_up, dense_down, mix_gate, norm_out,
):
    ep = lax.axis_size("ep")
    tp = lax.axis_size("tp")
    seqs, width = tokens.shape
    head_dim, length = cache_keys.shape[2:]
    chunks = 4
    topk = routes.shape[1]
    capacity = max(2, -(-seqs * topk // ep))
    slots = 8
    while slots < capacity:
        slots *= 2
    hidden_units = expert_gate.shape[2]
    rows = dense_gate.shape[0]
    share = dense_gate.shape[1] // tp
    flat_cache = (seqs * head_dim, length)
    total = ep * slots
    vmem = pl.BlockSpec(memory_space=pltpu.VMEM)
    smem = pl.BlockSpec(memory_space=pltpu.SMEM)
    hbm = pl.BlockSpec(memory_space=pl.ANY)
    half = width // 2
    dma = pltpu.SemaphoreType.DMA
    combined, fresh_k, fresh_v = pl.pallas_call(
        functools.partial(layer_kernel, ep, slots, chunks, head_dim),
        out_shape=(
            jax.ShapeDtypeStruct((seqs, width), F32),
            jax.ShapeDtypeStruct((seqs, w_key.shape[1]), BF16),
            jax.ShapeDtypeStruct((seqs, w_value.shape[1]), BF16),
        ),
        in_specs=[vmem] * 6 + [smem] * 2 + [hbm] * 12,
        out_specs=(vmem, vmem, vmem),
        scratch_shapes=[
            pltpu.VMEM(w_query.shape, BF16),
            pltpu.VMEM(w_key.shape[::-1], BF16),
            pltpu.VMEM(w_value.shape[::-1], BF16),
            pltpu.VMEM(flat_cache, BF16),
            pltpu.VMEM(flat_cache, BF16),
            pltpu.VMEM(w_output.shape, BF16),
            pltpu.VMEM((width, hidden_units), BF16),
            pltpu.VMEM((width, hidden_units), BF16),
            pltpu.VMEM((hidden_units, width), BF16),
            pltpu.VMEM((share, dense_down.shape[1]), BF16),
            pltpu.VMEM((3, rows, share), BF16),
            pltpu.VMEM((3, ep * rows, share), BF16),
            pltpu.VMEM((seqs, width), F32),
            pltpu.VMEM((seqs, width), F32),
            pltpu.VMEM((seqs, width), BF16),
            *[pltpu.VMEM((total, half), BF16)] * 7,
            pltpu.VMEM((seqs, width), F32),
            pltpu.VMEM((seqs, width), F32),
            dma((10 + 2 * chunks,)),
            dma((3,)),
            dma((3 * ep,)),
            dma((3 * ep,)),
            dma((ep,)),
            dma((ep,)),
            dma((ep,)),
            dma((ep,)),
            dma((4,)),
            dma((4,)),
        ],
        compiler_params=pltpu.CompilerParams(
            collective_id=0, has_side_effects=True, vmem_limit_bytes=60 * 1024 * 1024
        ),
    )(
        tokens,
        norm_in.reshape(1, width),
        norm_mid.reshape(1, width),
        mix_gate.reshape(1, width),
        routes.T,
        route_weights.T,
        cache_lengths,
        stick_bias,
        w_query,
        w_key.T,
        w_value.T,
        cache_keys.reshape(flat_cache),
        cache_values.reshape(flat_cache),
        w_output,
        expert_gate.reshape(width, hidden_units),
        expert_up.reshape(width, hidden_units),
        expert_down.reshape(hidden_units, width),
        dense_gate,
        dense_up,
        dense_down,
    )
    return pl.pallas_call(
        finish_kernel,
        out_shape=(
            jax.ShapeDtypeStruct((seqs, width), BF16),
            jax.ShapeDtypeStruct(fresh_k.shape, BF16),
            jax.ShapeDtypeStruct(fresh_v.shape, BF16),
        ),
    )(combined, norm_out.reshape(1, width), fresh_k, fresh_v)


def solution(mesh):
    in_specs = (
        P("ep", None),
        P("ep", "tp", None, None),
        P("ep", "tp", None, None),
        P("ep"),
        P(),
        P(None, "tp"),
        P(None, "tp"),
        P(None, "tp"),
        P("tp"),
        P("tp", None),
        P(),
        P("ep", None),
        P("ep", None),
        P("ep", None, "tp"),
        P("ep", None, "tp"),
        P("ep", "tp", None),
        P("ep", None),
        P("ep", None),
        P(None, "ep"),
        P(),
        P(),
    )
    out_specs = (P("ep", None), P("ep", "tp"), P("ep", "tp"))
    return jax.shard_map(shards, mesh=mesh, in_specs=in_specs, out_specs=out_specs, check_vma=False)
```

```python
import functools

import jax
import jax.numpy as jnp
from jax import lax
from jax.experimental import pallas as pl
from jax.experimental.pallas import tpu as pltpu
from jax.sharding import PartitionSpec as P

MESH = pl.DeviceIdType.MESH
F32 = jnp.float32
BF16 = jnp.bfloat16
LANES = 128
PLAN = ((3, 4, 5), (3, 4, 5), (2, 3, 4))


def layer_norm(values, gain):
    center = jnp.mean(values, -1, keepdims=True)
    spread = jnp.mean(jnp.square(values - center), -1, keepdims=True)
    return (values - center) * lax.rsqrt(spread + 1e-05) * gain


def sigmoid(x):
    return 1.0 / (1.0 + jnp.exp(-x))


def iota(shape, dim):
    return lax.broadcasted_iota(jnp.int32, shape, dim)


def bits(n):
    assert n & (n - 1) == 0
    return n.bit_length() - 1


def dot(a, b):
    return jnp.dot(a, b, preferred_element_type=F32)


def dot_nt(a, b):
    return lax.dot_general(a, b, (((1,), (1,)), ((), ())), preferred_element_type=F32)


def dot_tn(a, b):
    return lax.dot_general(a, b, (((0,), (0,)), ((), ())), preferred_element_type=F32)


def layer_kernel(
    ep, slots, chunks, head_dim,
    tokens, norm_in, norm_mid, mix_gate, routes, route_weights, lengths, bias,
    wq, wk, wv, keys, values, wo, eg, eu, ed, dg, du, dd,
    combined, fresh_k, fresh_v,
    wq_v, wk_v, wv_v, k_v, v_v, wo_v, eg_v, eu_v, ed_v, dd_v,
    pack, gath, proj_out, proj_in, hid_v, outgoing, received, received_other, part_out, part_in,
    expert_y, returned, fin_out, fin_in,
    load_sem, own_sem, gs, gr, ds, dr, rs, rr, ts, tr,
):
    me = lax.axis_index("ep")
    core = lax.axis_index("tp")
    other = 1 - core
    seqs, width = tokens.shape
    heads = bias.shape[0]
    length = keys.shape[1]
    rows = dg.shape[0]
    share = pack.shape[2]

    barrier = pltpu.get_barrier_semaphore()

    half = width // 2
    mine = pl.ds(pl.multiple_of(core * half, half), half)
    theirs = pl.ds(pl.multiple_of(other * half, half), half)

    def greet(p, c):
        pl.semaphore_signal(
            barrier, inc=1, device_id=(lax.rem(me + p, ep), core), device_id_type=MESH
        )
        return c

    lax.fori_loop(1, ep, greet, 0)
    pl.semaphore_signal(barrier, inc=1, device_id=(me, other), device_id_type=MESH)

    offset = pl.multiple_of(core * share, share)
    span = keys.shape[0] // chunks
    moves = [
        (dd.at[pl.ds(offset, share), :], dd_v),
        (dg.at[:, pl.ds(offset, share)], pack.at[0]),
        (du.at[:, pl.ds(offset, share)], pack.at[1]),
        (wq, wq_v),
    ]
    moves += [(keys.at[pl.ds(c * span, span)], k_v.at[pl.ds(c * span, span)]) for c in range(chunks)]
    moves += [(values.at[pl.ds(c * span, span)], v_v.at[pl.ds(c * span, span)]) for c in range(chunks)]
    moves += [(wo, wo_v), (wk, wk_v), (wv, wv_v), (eg, eg_v), (eu, eu_v), (ed, ed_v)]
    loads = [pltpu.make_async_copy(a, b, load_sem.at[i]) for i, (a, b) in enumerate(moves)]
    for load in loads:
        load.start()
    key_loads = loads[4 : 4 + chunks]
    value_loads = loads[4 + chunks : 4 + 2 * chunks]
    wo_load, wk_load, wv_load, eg_load, eu_load, ed_load = loads[4 + 2 * chunks :]

    normed = layer_norm(tokens[...].astype(F32), norm_in[...]).astype(BF16)

    total = ep * slots
    slot_of = iota((total, seqs), 0)
    expert_of = lax.shift_right_logical(slot_of, bits(slots))
    place_of = slot_of & (slots - 1)
    route_rows = routes[...]
    weight_rows = route_weights[...]
    member = jnp.zeros((total, seqs), F32)
    weight = jnp.zeros((total, seqs), F32)
    for k in range(route_rows.shape[0]):
        hit = route_rows[k : k + 1, :] == expert_of
        member = jnp.where(hit, 1.0, member)
        weight = jnp.where(hit, weight_rows[k : k + 1, :], weight)
    earlier = jnp.where(iota((seqs, seqs), 0) < iota((seqs, seqs), 1), 1.0, 0.0).astype(BF16)
    before = dot(member.astype(BF16), earlier).astype(jnp.int32)
    chosen = jnp.where(before == place_of, member, 0.0)
    weight = (weight * chosen).T
    chosen = chosen.astype(BF16)
    w_hi = weight.astype(BF16)
    w_rest = weight - w_hi.astype(F32)
    w_mid = w_rest.astype(BF16)
    w_lo = (w_rest - w_mid.astype(F32)).astype(BF16)
    weight_split = jnp.concatenate([w_hi, w_mid, w_lo], axis=0)

    grid_rows = heads * seqs
    flat = heads * head_dim
    col = iota((flat, heads * LANES), 1)
    spread_table = jnp.where(
        iota((flat, heads * LANES), 0)
        == lax.shift_right_logical(col, bits(LANES)) * head_dim + (col & (head_dim - 1)),
        1.0,
        0.0,
    ).astype(BF16)
    own_block = (
        lax.shift_right_logical(iota((grid_rows, seqs * head_dim), 1), bits(head_dim))
        == (iota((grid_rows, seqs * head_dim), 0) & (seqs - 1))
    )
    row = iota((2 * LANES, 2 * LANES), 0) & (LANES - 1)
    column = iota((2 * LANES, 2 * LANES), 1)
    later_table = jnp.where((column >= LANES) | (row > column), 1.0, 0.0).astype(BF16)
    row_seq = iota((grid_rows, 1), 0) & (seqs - 1)
    row_head = lax.shift_right_logical(iota((grid_rows, 1), 0), bits(seqs))
    filled = jnp.zeros((grid_rows, 1), jnp.int32)
    for s in range(seqs):
        filled = jnp.where(row_seq == s, lengths[s], filled)
    row_bias = jnp.zeros((grid_rows, 1), F32)
    for h in range(heads):
        row_bias = jnp.where(row_head == h, bias[h], row_bias)

    for load in loads[:3]:
        load.wait()
    pack[2] = dd_v[...].astype(F32).T.astype(BF16)

    def block(index, size):
        return pl.ds(pl.multiple_of(index * size, size), size)

    pl.semaphore_wait(barrier, ep)

    levels = bits(ep)
    my_bits = [lax.rem(me // (1 << k), 2) for k in range(levels)]

    def flip(mask):
        index = me
        for k in range(levels):
            if mask >> k & 1:
                index = index + (1 - 2 * my_bits[k]) * (1 << k)
        return index

    down = list(reversed(range(levels)))
    orders = [down, down[:-2] + [0, 1], [0, 1] + down[:-2]]
    steps = [[] for _ in range(levels)]
    number = 0
    for array, order in enumerate(orders):
        held = [0]
        for step, bit in enumerate(order):
            for mask in held:
                steps[step].append((number, array, mask, mask | 1 << bit, 1 << bit))
                number += 1
            held = held + [mask | 1 << bit for mask in held]

    def gather(item, incoming):
        number, array, mask, far_mask, bit = item
        return pltpu.make_async_remote_copy(
            src_ref=gath.at[array, block(flip(mask), rows), :] if mask else pack.at[array],
            dst_ref=gath.at[array, block(flip(far_mask if incoming else mask), rows), :],
            send_sem=gs.at[number],
            recv_sem=gr.at[number],
            device_id=(flip(bit), core),
            device_id_type=MESH,
        )

    def gather_start(step):
        for item in steps[step]:
            gather(item, False).start()

    def gather_wait(step):
        for item in steps[step]:
            gather(item, True).wait_recv()

    def advance(point):
        for step in range(1, levels):
            for array, plan in enumerate(PLAN):
                if plan[min(step - 1, len(plan) - 1)] == point:
                    for item in steps[step - 1]:
                        if item[1] == array:
                            gather(item, True).wait_recv()
                    for item in steps[step]:
                        if item[1] == array:
                            gather(item, False).start()

    gather_start(0)
    own_gather = pltpu.make_async_copy(pack, gath.at[:, block(me, rows), :], own_sem.at[0])
    own_gather.start()

    loads[3].wait()
    queries = dot(normed, wq_v[...]).astype(BF16)
    twice = dot(queries, spread_table)
    stacked = jnp.concatenate([twice[:, h * LANES : (h + 1) * LANES] for h in range(heads)], axis=0)
    tiled = jnp.concatenate([stacked] * (seqs * head_dim // LANES), axis=1)
    query_grid = jnp.where(own_block, tiled, 0.0).astype(BF16)
    scores = None
    for c in range(chunks):
        key_loads[c].wait()
        part = dot(query_grid[:, c * span : (c + 1) * span], k_v[c * span : (c + 1) * span, :])
        scores = part if scores is None else scores + part
    advance(1)
    scores = scores * head_dim ** (-0.5) + row_bias
    visible = iota((grid_rows, length), 1) < filled
    soft = jnp.log1p(jnp.exp(-jnp.abs(scores)))
    log_keep = jnp.where(visible, jnp.minimum(-scores, 0.0) - soft, 0.0)
    log_take = jnp.minimum(scores, 0.0) - soft
    count = length // LANES
    keep_hi = log_keep.astype(BF16).astype(F32)
    keep_lo = log_keep - keep_hi
    stack = jnp.concatenate(
        [
            jnp.concatenate(
                [keep_hi[:, c * LANES : (c + 1) * LANES], keep_lo[:, c * LANES : (c + 1) * LANES]], axis=1
            )
            for c in range(count)
        ],
        axis=0,
    ).astype(BF16)
    sums = dot(stack, later_table)
    carried = jnp.zeros((grid_rows, LANES), F32)
    pieces = [None] * count
    for c in reversed(range(count)):
        here = sums[c * grid_rows : (c + 1) * grid_rows]
        pieces[c] = here[:, :LANES] + carried
        carried = carried + here[:, LANES:]
    later = jnp.concatenate(pieces, axis=1)
    stick = jnp.where(visible, jnp.exp(log_take + later), 0.0).astype(BF16)
    advance(2)
    folded = jnp.zeros((grid_rows, LANES), F32)
    for c in range(chunks):
        value_loads[c].wait()
        part = dot_nt(stick, v_v[c * span : (c + 1) * span, :])
        part = jnp.where(own_block[:, c * span : (c + 1) * span], part, 0.0)
        for b in range(span // LANES):
            folded = folded + part[:, b * LANES : (b + 1) * LANES]
    folded = jnp.concatenate([folded[h * seqs : (h + 1) * seqs] for h in range(heads)], axis=1)
    attended = dot_nt(folded.astype(BF16), spread_table).astype(BF16)
    wo_load.wait()
    part_proj = dot(attended, wo_v[...])
    proj_out[...] = part_proj

    def swap(index, source, target):
        return pltpu.make_async_remote_copy(
            src_ref=source,
            dst_ref=target,
            send_sem=ts.at[index],
            recv_sem=tr.at[index],
            device_id=(me, other),
            device_id_type=MESH,
        )

    proj_swap = swap(0, proj_out, proj_in)
    proj_swap.start()
    advance(3)
    wk_load.wait()
    fresh_k[...] = dot_nt(normed, wk_v[...]).astype(BF16)
    wv_load.wait()
    fresh_v[...] = dot_nt(normed, wv_v[...]).astype(BF16)
    proj_swap.wait()
    projected = part_proj + proj_in[...]
    hidden = layer_norm(normed.astype(F32) + projected, norm_mid[...]).astype(BF16)

    hid_v[...] = hidden
    outgoing[...] = dot(chosen, hid_v[:, mine]).astype(BF16)

    def dispatch(p, source, target):
        return pltpu.make_async_remote_copy(
            src_ref=outgoing.at[block(source, slots), :],
            dst_ref=received.at[block(target, slots), :],
            send_sem=ds.at[p],
            recv_sem=dr.at[p],
            device_id=(lax.rem(me + p, ep), core),
            device_id_type=MESH,
        )

    def start_dispatch(p, c):
        dispatch(p, lax.rem(me + p, ep), me).start()
        return c

    lax.fori_loop(1, ep, start_dispatch, 0)
    own_rows = pltpu.make_async_copy(
        outgoing.at[block(me, slots), :], received.at[block(me, slots), :], own_sem.at[1]
    )
    own_rows.start()

    hidden_f = hidden.astype(F32)
    mix_weight = sigmoid(jnp.sum(hidden_f * mix_gate[...], axis=-1, keepdims=True))

    advance(4)

    eg_load.wait()
    eu_load.wait()
    ed_load.wait()

    def wait_dispatch(p, c):
        source = lax.rem(me + ep - p, ep)
        done = dispatch(p, lax.rem(me + p, ep), source)
        done.wait_recv()
        done.wait_send()
        return c

    lax.fori_loop(1, ep, wait_dispatch, 0)
    own_rows.wait()
    row_swap = swap(2, received, received_other)
    row_swap.start()
    advance(5)
    near = received[...]
    gate_pre = dot(near, eg_v[mine, :])
    up_pre = dot(near, eu_v[mine, :])
    row_swap.wait()
    far = received_other[...]
    gate_pre = gate_pre + dot(far, eg_v[theirs, :])
    up_pre = up_pre + dot(far, eu_v[theirs, :])
    act = (gate_pre * sigmoid(gate_pre) * up_pre).astype(BF16)
    part_out[...] = dot(act, ed_v[:, theirs]).astype(BF16)
    part_swap = swap(3, part_out, part_in)
    part_swap.start()
    advance(6)
    own_part = dot(act, ed_v[:, mine]).astype(BF16).astype(F32)
    part_swap.wait()
    expert_y[...] = (own_part + part_in[...].astype(F32)).astype(BF16)

    def give_back(p, source, target):
        return pltpu.make_async_remote_copy(
            src_ref=expert_y.at[block(source, slots), :],
            dst_ref=returned.at[block(target, slots), :],
            send_sem=rs.at[p],
            recv_sem=rr.at[p],
            device_id=(lax.rem(me + p, ep), core),
            device_id_type=MESH,
        )

    def start_return(p, c):
        give_back(p, lax.rem(me + p, ep), me).start()
        return c

    lax.fori_loop(1, ep, start_return, 0)
    own_back = pltpu.make_async_copy(
        expert_y.at[block(me, slots), :], returned.at[block(me, slots), :], own_sem.at[2]
    )
    own_back.start()
    advance(7)
    gather_wait(levels - 1)
    for step in range(levels):
        for item in steps[step]:
            gather(item, False).wait_send()
    own_gather.wait()
    dense_pre = dot(hidden, gath[0])
    dense_lin = dot(hidden, gath[1])
    dense_act = (dense_pre * sigmoid(dense_pre) * dense_lin).astype(BF16)
    dense_part = dot_nt(dense_act, gath[2]) * mix_weight


    def wait_return(p, c):
        source = lax.rem(me + ep - p, ep)
        done = give_back(p, lax.rem(me + p, ep), source)
        done.wait_recv()
        done.wait_send()
        return c

    lax.fori_loop(1, ep, wait_return, 0)
    own_back.wait()
    routed3 = dot(weight_split, returned[...])
    routed = routed3[:seqs] + routed3[seqs : 2 * seqs] + routed3[2 * seqs :]
    fin_out[...] = dense_part
    fin_out[:, mine] = fin_out[:, mine] + routed
    fin_swap = swap(1, fin_out, fin_in)
    fin_swap.start()
    fin_swap.wait()
    combined[...] = hidden_f + (fin_out[...] + fin_in[...])


def finish_kernel(combined, norm_out, fresh_k, fresh_v, mixed, out_k, out_v):
    mixed[...] = layer_norm(combined[...], norm_out[...]).astype(BF16)
    out_k[...] = fresh_k[...]
    out_v[...] = fresh_v[...]


def shards(
    tokens, cache_keys, cache_values, cache_lengths, norm_in, w_query, w_key, w_value, stick_bias,
    w_output, norm_mid, routes, route_weights, expert_gate, expert_up, expert_down,
    dense_gate, dense_up, dense_down, mix_gate, norm_out,
):
    ep = lax.axis_size("ep")
    tp = lax.axis_size("tp")
    seqs, width = tokens.shape
    head_dim, length = cache_keys.shape[2:]
    chunks = 4
    topk = routes.shape[1]
    capacity = max(2, -(-seqs * topk // ep))
    slots = 8
    while slots < capacity:
        slots *= 2
    hidden_units = expert_gate.shape[2]
    rows = dense_gate.shape[0]
    share = dense_gate.shape[1] // tp
    flat_cache = (seqs * head_dim, length)
    total = ep * slots
    vmem = pl.BlockSpec(memory_space=pltpu.VMEM)
    smem = pl.BlockSpec(memory_space=pltpu.SMEM)
    hbm = pl.BlockSpec(memory_space=pl.ANY)
    half = width // 2
    dma = pltpu.SemaphoreType.DMA
    combined, fresh_k, fresh_v = pl.pallas_call(
        functools.partial(layer_kernel, ep, slots, chunks, head_dim),
        out_shape=(
            jax.ShapeDtypeStruct((seqs, width), F32),
            jax.ShapeDtypeStruct((seqs, w_key.shape[1]), BF16),
            jax.ShapeDtypeStruct((seqs, w_value.shape[1]), BF16),
        ),
        in_specs=[vmem] * 6 + [smem] * 2 + [hbm] * 12,
        out_specs=(vmem, vmem, vmem),
        scratch_shapes=[
            pltpu.VMEM(w_query.shape, BF16),
            pltpu.VMEM(w_key.shape[::-1], BF16),
            pltpu.VMEM(w_value.shape[::-1], BF16),
            pltpu.VMEM(flat_cache, BF16),
            pltpu.VMEM(flat_cache, BF16),
            pltpu.VMEM(w_output.shape, BF16),
            pltpu.VMEM((width, hidden_units), BF16),
            pltpu.VMEM((width, hidden_units), BF16),
            pltpu.VMEM((hidden_units, width), BF16),
            pltpu.VMEM((share, dense_down.shape[1]), BF16),
            pltpu.VMEM((3, rows, share), BF16),
            pltpu.VMEM((3, ep * rows, share), BF16),
            pltpu.VMEM((seqs, width), F32),
            pltpu.VMEM((seqs, width), F32),
            pltpu.VMEM((seqs, width), BF16),
            *[pltpu.VMEM((total, half), BF16)] * 7,
            pltpu.VMEM((seqs, width), F32),
            pltpu.VMEM((seqs, width), F32),
            dma((10 + 2 * chunks,)),
            dma((3,)),
            dma((3 * ep,)),
            dma((3 * ep,)),
            dma((ep,)),
            dma((ep,)),
            dma((ep,)),
            dma((ep,)),
            dma((4,)),
            dma((4,)),
        ],
        compiler_params=pltpu.CompilerParams(
            collective_id=0, has_side_effects=True, vmem_limit_bytes=60 * 1024 * 1024
        ),
    )(
        tokens,
        norm_in.reshape(1, width),
        norm_mid.reshape(1, width),
        mix_gate.reshape(1, width),
        routes.T,
        route_weights.T,
        cache_lengths,
        stick_bias,
        w_query,
        w_key.T,
        w_value.T,
        cache_keys.reshape(flat_cache),
        cache_values.reshape(flat_cache),
        w_output,
        expert_gate.reshape(width, hidden_units),
        expert_up.reshape(width, hidden_units),
        expert_down.reshape(hidden_units, width),
        dense_gate,
        dense_up,
        dense_down,
    )
    return pl.pallas_call(
        finish_kernel,
        out_shape=(
            jax.ShapeDtypeStruct((seqs, width), BF16),
            jax.ShapeDtypeStruct(fresh_k.shape, BF16),
            jax.ShapeDtypeStruct(fresh_v.shape, BF16),
        ),
    )(combined, norm_out.reshape(1, width), fresh_k, fresh_v)


def solution(mesh):
    in_specs = (
        P("ep", None),
        P("ep", "tp", None, None),
        P("ep", "tp", None, None),
        P("ep"),
        P(),
        P(None, "tp"),
        P(None, "tp"),
        P(None, "tp"),
        P("tp"),
        P("tp", None),
        P(),
        P("ep", None),
        P("ep", None),
        P("ep", None, "tp"),
        P("ep", None, "tp"),
        P("ep", "tp", None),
        P("ep", None),
        P("ep", None),
        P(None, "ep"),
        P(),
        P(),
    )
    out_specs = (P("ep", None), P("ep", "tp"), P("ep", "tp"))
    return jax.shard_map(shards, mesh=mesh, in_specs=in_specs, out_specs=out_specs, check_vma=False)
```
